32 devices in a mesh: sp: 8 (over z, x), tp: 4 (over y, core).
Axes of the slice: x: 2, y: 2, z: 4, core: 2. Of those that a mesh axis runs over, the one named last changes fastest.
Arguments:
- tokens: bfloat16 [6144, 2048], P('sp', 'tp'), may hold values from -23 to 23, as said below
- norm_gain: float32 [2048], replicated, may hold values from 0.8 to 8, as said below
- window_query: bfloat16 [2048, 1024], P(None, 'tp'), may hold values from -0.125 to 0.125
- window_key: bfloat16 [2048, 512], P(None, 'tp'), may hold values from -0.125 to 0.125
- window_value: bfloat16 [2048, 512], P(None, 'tp'), may hold values from -0.125 to 0.125
- sink_logit: float32 [16], P('tp'), may hold values from 2 to 6
- down_query: bfloat16 [2048, 768], replicated, may hold values from -0.125 to 0.125
- down_latent: bfloat16 [2048, 512], replicated, may hold values from -0.125 to 0.125
- rotary_proj: bfloat16 [2048, 32], replicated, may hold values from -0.125 to 0.125
- query_gain: float32 [768], replicated, may hold values from 0.8 to 8, as said below
- latent_gain: float32 [512], replicated, may hold values from 0.8 to 8, as said below
- up_query: bfloat16 [768, 1536], P(None, 'tp'), may hold values from -0.21875 to 0.21875
- up_key: bfloat16 [512, 1024], P(None, 'tp'), may hold values from -0.25 to 0.25
- up_value: bfloat16 [512, 1024], P(None, 'tp'), may hold values from -0.25 to 0.25
- window_out: bfloat16 [1024, 2048], P('tp'), may hold values from -0.125 to 0.125
- latent_out: bfloat16 [1024, 2048], P('tp'), may hold values from -0.125 to 0.125
Outputs:
- mixed: bfloat16 [6144, 2048], P(('sp', 'tp'))
The draws below stay inside these ranges and needn't reach their ends.
Inputs may be any that keep to these rules, and one draw needn't show every extreme that they name: `tokens`: real-valued; the channels carry scales that vary smoothly by a factor of up to twenty across the width. `norm_gain`: positive. `query_gain`: positive. `latent_gain`: positive.
All inputs are finite; a program needn't handle non-finite values.
Results may differ from the reference program's by a relative error of at most 0.04.
The reference program's roundings to bfloat16 on the way count: a program that leaves them out, or rounds other values in their place, can miss the bound.
Values may be sent and summed in bfloat16 or wider, within the bound.
No kernel may reach another device: no remote copies, remote signals or barrier semaphores. Data moves between devices by JAX's collectives and lax.ppermute only.
A program may use at most 128 MiB of HBM per device.

```python
import jax
import jax.numpy as jnp
from jax import lax

D = 2048
A_HEADS = 16
KV_HEADS = 8
HD = 64
B_HEADS = 16
NOPE = 64
ROPE = 32
VD = 64
QRANK = 768
KVRANK = 512
WINDOW = 128
QBLOCK = 256
TOKENS = 6144
N_TP = 4


def gain_values(key, length):
    return jax.random.uniform(key, (length,), jnp.float32, 0.8, 2.4)


def draw_norm_gain(key, part):
    return gain_values(jax.random.fold_in(key, 11), D)


def draw_query_gain(key, part):
    return gain_values(jax.random.fold_in(key, 13), QRANK)


def draw_latent_gain(key, part):
    return gain_values(jax.random.fold_in(key, 17), KVRANK)


def draw_tokens(key, part):
    phase = jax.random.uniform(jax.random.fold_in(key, 3), (), jnp.float32, 0.0, 6.2831853)
    channel = jnp.arange(D, dtype=jnp.float32)
    channel_scale = jnp.exp(1.5 * jnp.cos(6.2831853 * channel / D + phase))
    base = jnp.clip(jax.random.normal(jax.random.fold_in(key, 7), (TOKENS, D), jnp.float32), -5.0, 5.0)
    return (base * channel_scale[None, :]).astype(jnp.bfloat16)


def block_scale(own_key, dims, pieces, low, top_value):
    gain, own = 1.0, jax.random.fold_in(own_key, 6)
    for axis_at, blocks in pieces:
        steps = jnp.exp(jax.random.uniform(jax.random.fold_in(own, axis_at), (blocks,), jnp.float32, low / len(pieces), top_value / len(pieces)))
        gain = gain * jnp.repeat(steps, dims[axis_at] // blocks).reshape([-1 if axis == axis_at else 1 for axis in range(len(dims))])
    return gain


def gaussian(key, extent, spread, reach, split=(), kind=jnp.bfloat16):
    array = jax.random.normal(key, extent, jnp.float32) * spread
    if len(split) > 0:
        array = block_scale(key, extent, split, -0.22, 0.18) * array
    return jnp.clip(array, min=-reach, max=reach).astype(kind)


def setup_inputs(seed: int = 0) -> dict:
    arg_keys = jax.random.split(jax.random.key(seed), 17)
    return {
        "tokens": draw_tokens(jax.random.fold_in(arg_keys[16], 71), 0),
        "norm_gain": draw_norm_gain(jax.random.fold_in(arg_keys[16], 71), 0),
        "window_query": gaussian(arg_keys[2], (D, A_HEADS * HD), D ** -0.5, 0.125, ((1, 4),)),
        "window_key": gaussian(arg_keys[3], (D, KV_HEADS * HD), D ** -0.5, 0.125, ((1, 4),)),
        "window_value": gaussian(arg_keys[4], (D, KV_HEADS * HD), D ** -0.5, 0.125, ((1, 4),)),
        "sink_logit": jnp.clip(2.0 + 4.0 * jax.random.uniform(arg_keys[5], (A_HEADS,), jnp.float32) ** block_scale(arg_keys[5], (A_HEADS,), ((0, 4),), -0.2, 0.2), 2.0, 6.0),
        "down_query": gaussian(arg_keys[6], (D, QRANK), D ** -0.5, 0.125),
        "down_latent": gaussian(arg_keys[7], (D, KVRANK), D ** -0.5, 0.125),
        "rotary_proj": gaussian(arg_keys[8], (D, ROPE), D ** -0.5, 0.125),
        "query_gain": draw_query_gain(jax.random.fold_in(arg_keys[16], 71), 0),
        "latent_gain": draw_latent_gain(jax.random.fold_in(arg_keys[16], 71), 0),
        "up_query": gaussian(arg_keys[11], (QRANK, B_HEADS * (NOPE + ROPE)), QRANK ** -0.5, 0.21875, ((1, 4),)),
        "up_key": gaussian(arg_keys[12], (KVRANK, B_HEADS * NOPE), KVRANK ** -0.5, 0.25, ((1, 4),)),
        "up_value": gaussian(arg_keys[13], (KVRANK, B_HEADS * VD), KVRANK ** -0.5, 0.25, ((1, 4),)),
        "window_out": gaussian(arg_keys[14], (A_HEADS * HD, D), (A_HEADS * HD + B_HEADS * VD) ** -0.5, 0.125, ((0, 4),)),
        "latent_out": gaussian(arg_keys[15], (B_HEADS * VD, D), (A_HEADS * HD + B_HEADS * VD) ** -0.5, 0.125, ((0, 4),)),
    }


EPS = 1e-06
THETA = 10000.0

def rotate(vector, positions):
    half_len = vector.shape[-1] // 2
    inverse = THETA ** (-jnp.arange(half_len, dtype=jnp.float32) / half_len)
    angles = positions.astype(jnp.float32)[:, None] * inverse[None, :]
    new_shape = (angles.shape[0],) + (1,) * (vector.ndim - 2) + (half_len,)
    cosine = jnp.cos(angles).reshape(new_shape)
    sine_part = jnp.sin(angles).reshape(new_shape)
    front_half = vector[..., :half_len].astype(jnp.float32)
    second = vector[..., half_len:].astype(jnp.float32)
    return jnp.concatenate([front_half * cosine - second * sine_part, second * cosine + front_half * sine_part], axis=-1)

def norm_rows(values, gain_vec):
    as_float = values.astype(jnp.float32)
    return (as_float * lax.rsqrt(lax.optimization_barrier(jnp.mean(as_float * as_float, axis=1, keepdims=True)) + EPS) * gain_vec).astype(jnp.bfloat16)

def window_attention(q_rows, key_rows, value_rows, sink_logit):
    row_count = q_rows.shape[0]
    group = A_HEADS // KV_HEADS
    padded_keys = jnp.pad(key_rows, ((WINDOW, WINDOW), (0, 0)))
    padded_values = jnp.pad(value_rows, ((WINDOW, WINDOW), (0, 0)))
    span_len = QBLOCK + 2 * WINDOW
    distance = jnp.arange(QBLOCK)[:, None] + WINDOW - jnp.arange(span_len)[None, :]
    slopes = jnp.exp2(-8.0 * (jnp.arange(A_HEADS, dtype=jnp.float32) + 1.0) / A_HEADS).reshape(KV_HEADS, group)
    sinks = sink_logit.astype(jnp.float32).reshape(KV_HEADS, group)[:, :, None, None]

    def one_block(offset):
        queries = lax.dynamic_slice_in_dim(q_rows, offset, QBLOCK, 0).astype(jnp.float32).reshape(QBLOCK, KV_HEADS, group, HD)
        key_part = lax.dynamic_slice_in_dim(padded_keys, offset, span_len, 0).astype(jnp.float32).reshape(span_len, KV_HEADS, HD)
        value_part = lax.dynamic_slice_in_dim(padded_values, offset, span_len, 0).astype(jnp.float32).reshape(span_len, KV_HEADS, HD)
        scores = jnp.einsum('qhgd,khd->hgqk', queries, key_part) * HD ** (-0.5)
        scores = scores - slopes[:, :, None, None] * jnp.abs(distance).astype(jnp.float32)
        key_pos = offset + jnp.arange(span_len, dtype=jnp.int32) - WINDOW
        valid = (jnp.abs(distance) <= WINDOW) & ((key_pos >= 0) & (key_pos < row_count))[None, :]
        scores = jnp.where(valid, scores, -jnp.inf)
        row_max = jnp.maximum(lax.optimization_barrier(jnp.max(scores, axis=3, keepdims=True)), sinks)
        weights = jnp.exp(scores - row_max)
        weights = weights / (lax.optimization_barrier(jnp.sum(weights, axis=3, keepdims=True)) + jnp.exp(sinks - row_max))
        rounded = lax.optimization_barrier(weights.astype(jnp.bfloat16)).astype(jnp.float32)
        return jnp.einsum('hgqk,khd->qhgd', rounded, value_part).astype(jnp.bfloat16).reshape(QBLOCK, A_HEADS * HD)
    offsets = (jnp.arange(row_count // QBLOCK) * QBLOCK).astype(jnp.int32)
    return lax.map(one_block, offsets).reshape(row_count, A_HEADS * HD)

def latent_attention(q_nope, q_rot, key_rows, value_rows, k_rot):
    row_count = q_nope.shape[0]
    lat_scale = (NOPE + ROPE) ** (-0.5)
    keys_float = key_rows.astype(jnp.float32)
    values_float = value_rows.astype(jnp.float32)
    krot_float = k_rot.astype(jnp.float32)

    def one_block(offset):
        q_part = lax.dynamic_slice_in_dim(q_nope, offset, QBLOCK, 0).astype(jnp.float32)
        rot_part = lax.dynamic_slice_in_dim(q_rot, offset, QBLOCK, 0).astype(jnp.float32)
        scores = (jnp.einsum('qhd,khd->hqk', q_part, keys_float) + jnp.einsum('qhr,kr->hqk', rot_part, krot_float)) * lat_scale
        row_max = lax.optimization_barrier(jnp.max(scores, axis=2, keepdims=True))
        weights = jnp.exp(scores - row_max)
        denom_sum = lax.optimization_barrier(jnp.sum(weights, axis=2))
        rounded = lax.optimization_barrier(weights.astype(jnp.bfloat16)).astype(jnp.float32)
        summed = jnp.einsum('hqk,khd->qhd', rounded, values_float)
        return (summed / denom_sum.T[:, :, None]).astype(jnp.bfloat16)
    offsets = (jnp.arange(row_count // QBLOCK) * QBLOCK).astype(jnp.int32)
    return lax.map(one_block, offsets).reshape(row_count, B_HEADS * VD)

def reference(tokens, norm_gain, window_query, window_key, window_value, sink_logit, down_query, down_latent, rotary_proj, query_gain, latent_gain, up_query, up_key, up_value, window_out, latent_out):
    row_count = tokens.shape[0]
    as_float = tokens.astype(jnp.float32)
    row_scale = lax.rsqrt(lax.optimization_barrier(jnp.mean(as_float * as_float, axis=1, keepdims=True)) + EPS)
    scaled = (as_float * norm_gain).astype(jnp.bfloat16)

    def project(weight):
        return (jnp.dot(scaled, weight, preferred_element_type=jnp.float32) * row_scale).astype(jnp.bfloat16)
    q_window = project(window_query)
    k_window = project(window_key)
    v_window = project(window_value)
    latent_q = project(down_query)
    latent_kv = project(down_latent)
    rotary_rows = project(rotary_proj)
    positions = jnp.arange(row_count, dtype=jnp.int32)
    out_window = window_attention(q_window, k_window, v_window, sink_logit)
    q_latent = jnp.dot(norm_rows(latent_q, query_gain), up_query, preferred_element_type=jnp.float32).astype(jnp.bfloat16)
    q_latent = q_latent.reshape(row_count, B_HEADS, NOPE + ROPE)
    normed_kv = norm_rows(latent_kv, latent_gain)
    key_rows = jnp.dot(normed_kv, up_key, preferred_element_type=jnp.float32).astype(jnp.bfloat16).reshape(row_count, B_HEADS, NOPE)
    value_rows = jnp.dot(normed_kv, up_value, preferred_element_type=jnp.float32).astype(jnp.bfloat16).reshape(row_count, B_HEADS, VD)
    q_nope = q_latent[..., :NOPE]
    q_rot = rotate(q_latent[..., NOPE:], positions).astype(jnp.bfloat16)
    k_rot = rotate(rotary_rows, positions).astype(jnp.bfloat16)
    out_latent = latent_attention(q_nope, q_rot, key_rows, value_rows, k_rot)
    a_share = A_HEADS * HD // N_TP
    b_share = B_HEADS * VD // N_TP
    summed = jnp.zeros((row_count, D), jnp.float32)
    for member in range(N_TP):
        head_part = jnp.dot(out_window[:, member * a_share:(member + 1) * a_share], window_out[member * a_share:(member + 1) * a_share], preferred_element_type=jnp.float32)
        head_part = head_part + jnp.dot(out_latent[:, member * b_share:(member + 1) * b_share], latent_out[member * b_share:(member + 1) * b_share], preferred_element_type=jnp.float32)
        summed = summed + lax.optimization_barrier(head_part.astype(jnp.bfloat16)).astype(jnp.float32)
    return summed.astype(jnp.bfloat16)
```

```python
import functools

import jax
import jax.numpy as jnp
from jax import lax
from jax.experimental import pallas as pl
from jax.experimental.pallas import tpu as pltpu
from jax.sharding import PartitionSpec as P

A_HEADS = 16
HD = 64
NOPE = 64
ROPE = 32
VD = 64
WINDOW = 128

EPS = 1e-06
THETA = 10000.0
LANES = 128
QCOLS = 256
NEG = -1e30
LOG2E = 1.4426950408889634
F32 = jnp.float32
BF16 = jnp.bfloat16


def swap(x, bit):
    size = lax.axis_size("tp")
    return lax.ppermute(x, "tp", [(i, i ^ bit) for i in range(size)])


def norm_rows(values, gain_vec):
    as_float = values.astype(F32)
    return (
        as_float * lax.rsqrt(jnp.mean(as_float * as_float, axis=1, keepdims=True) + EPS) * gain_vec
    ).astype(BF16)


def angle_table(positions, half_len):
    inverse = THETA ** (-jnp.arange(half_len, dtype=F32) / half_len)
    angles = inverse[:, None] * positions.astype(F32)[None, :]
    return jnp.cos(angles), jnp.sin(angles)


def flash_kernel(scale, chunk, run, started, last, *refs):
    refs = list(refs)
    k_ref, rot_ref, v_ref, q_ref = refs[:4]
    state = refs[4:6] if started else None
    outs = refs[4 + (2 if started else 0) : -2]
    keys, values_t = refs[-2:]

    @pl.when(lax.rem(pl.program_id(0), run) == 0)
    def _():
        keys[:, :LANES] = k_ref[...]
        keys[:, LANES:] = rot_ref[...]
        values_t[...] = v_ref[...].T

    count = keys.shape[0] // chunk
    factor = scale * LOG2E
    q = q_ref[...]

    def score(i):
        return jnp.dot(keys[i * chunk : (i + 1) * chunk, :], q, preferred_element_type=F32)

    top = total = acc = None
    if started:
        top, total, acc = state[0][0:1, :], state[0][1:2, :], state[1][...]
    pending = score(0)
    for i in range(count):
        s = pending
        if i + 1 < count:
            pending = score(i + 1)
        best = jnp.max(s, axis=0, keepdims=True)
        new_top = best if top is None else jnp.maximum(top, best)
        p = jnp.exp2(s * factor - new_top * factor)
        part = jnp.sum(p, axis=0, keepdims=True)
        mixed = jnp.dot(
            values_t[:, i * chunk : (i + 1) * chunk], p.astype(BF16), preferred_element_type=F32
        )
        if top is None:
            total, acc = part, mixed
        else:
            rescale = jnp.exp2((top - new_top) * factor)
            total = total * rescale + part
            acc = acc * rescale + mixed
        top = new_top
    if last:
        outs[0][...] = (acc / total).T.astype(BF16)
    else:
        outs[0][0:1, :] = top
        outs[0][1:2, :] = total
        outs[1][...] = acc


def flash(keys, rot, values, q_cols, state, pairs, chunk, scale, base=0, cols=None):
    last = cols is not None
    rows, cols = keys.shape[0], cols or q_cols.shape[1]
    step = QCOLS
    run = q_cols.shape[1] // (2 * pairs * step)
    first = base // step
    pair = lambda n: (0, lax.rem(lax.div(n, run), pairs))
    column = lambda n: (0, n + first)
    in_specs = [
        pl.BlockSpec((rows, LANES), pair),
        pl.BlockSpec((rows, LANES), lambda n: (0, 0)),
        pl.BlockSpec((rows, LANES), pair),
        pl.BlockSpec((2 * LANES, step), column),
    ]
    if state is not None:
        in_specs += [pl.BlockSpec((8, step), column), pl.BlockSpec((LANES, step), column)]
    if last:
        out_specs = pl.BlockSpec((step, LANES), lambda n: (n, 0))
        out_shape = jax.ShapeDtypeStruct((cols, LANES), BF16)
    else:
        out_specs = [pl.BlockSpec((8, step), column), pl.BlockSpec((LANES, step), column)]
        out_shape = [
            jax.ShapeDtypeStruct((8, cols), F32),
            jax.ShapeDtypeStruct((LANES, cols), F32),
        ]
    return pl.pallas_call(
        functools.partial(flash_kernel, scale, chunk, run, state is not None, last),
        grid=(cols // step,),
        in_specs=in_specs,
        out_specs=out_specs,
        out_shape=out_shape,
        scratch_shapes=[pltpu.VMEM((rows, 2 * LANES), BF16), pltpu.VMEM((LANES, rows), BF16)],
        compiler_params=pltpu.CompilerParams(
            dimension_semantics=("arbitrary",), vmem_limit_bytes=40 * 1024 * 1024
        ),
        cost_estimate=pl.CostEstimate(
            flops=2 * rows * cols * 4 * LANES,
            transcendentals=rows * cols,
            bytes_accessed=rows * 5 * LANES * 2 + cols * 8 * LANES,
        ),
        name="latent_flash",
    )(keys, rot, values, q_cols, *(state or ()))


def window_kernel(
    heads, kv_heads, half, info_ref, slope_ref, sink_ref, q_ref, k_ref, v_ref, out_ref
):
    which = info_ref[pl.program_id(0)]
    base = pl.multiple_of(which * half, half)
    span = half + 2 * WINDOW
    keys = k_ref[pl.ds(base, span), :]
    values_t = v_ref[pl.ds(base, span), :].T
    q_t = q_ref[...].T
    row = lax.broadcasted_iota(jnp.int32, (span, half), 0)
    col = lax.broadcasted_iota(jnp.int32, (span, half), 1)
    distance = jnp.abs(col + WINDOW - row)
    key_pos = info_ref[2] + base + row - WINDOW
    valid = (distance <= WINDOW) & (key_pos >= 0) & (key_pos < info_ref[3])
    apart = distance.astype(F32)
    group = heads // kv_heads
    outs = []
    for h in range(heads):
        g = h // group
        mine = q_t[h * HD : (h + 1) * HD, :]
        pieces = [mine if i == g else jnp.zeros_like(mine) for i in range(kv_heads)]
        weight = pieces[0] if kv_heads == 1 else jnp.concatenate(pieces, axis=0)
        s = jnp.dot(keys, weight, preferred_element_type=F32) * HD ** (-0.5)
        s = jnp.where(valid, s - slope_ref[h] * apart, NEG)
        sink = sink_ref[h]
        top = jnp.maximum(jnp.max(s, axis=0, keepdims=True), sink)
        p = jnp.exp(s - top)
        denom = jnp.sum(p, axis=0, keepdims=True) + jnp.exp(sink - top)
        p = (p * (1.0 / denom)).astype(BF16)
        mixed = jnp.dot(values_t, p, preferred_element_type=F32)
        outs.append(mixed[g * HD : (g + 1) * HD, :])
    out_ref[...] = jnp.concatenate(outs, axis=0).T.astype(BF16)


def window_attention(q, k_pad, v_pad, info, slopes, sinks):
    rows, width = q.shape
    half = rows // 2
    heads, kv_heads = width // HD, k_pad.shape[1] // HD
    whole = lambda n, info: (0, 0)
    smem = pl.BlockSpec(memory_space=pltpu.SMEM)
    return pl.pallas_call(
        functools.partial(window_kernel, heads, kv_heads, half),
        grid_spec=pltpu.PrefetchScalarGridSpec(
            num_scalar_prefetch=1,
            grid=(2,),
            in_specs=[
                smem,
                smem,
                pl.BlockSpec((half, width), lambda n, info: (info[n], 0)),
                pl.BlockSpec(k_pad.shape, whole),
                pl.BlockSpec(v_pad.shape, whole),
            ],
            out_specs=pl.BlockSpec((half, width), lambda n, info: (n, 0)),
        ),
        out_shape=jax.ShapeDtypeStruct((rows, width), BF16),
        compiler_params=pltpu.CompilerParams(
            dimension_semantics=("arbitrary",), vmem_limit_bytes=40 * 1024 * 1024
        ),
        cost_estimate=pl.CostEstimate(
            flops=8 * rows * 640 * width,
            transcendentals=rows * 640 * heads,
            bytes_accessed=rows * width * 8,
        ),
        name="window_flash",
    )(info, slopes, sinks, q, k_pad, v_pad)


def per_device(
    tokens,
    norm_gain,
    window_query,
    window_key,
    window_value,
    sink_logit,
    down_query,
    down_latent,
    rotary_proj,
    query_gain,
    latent_gain,
    up_query,
    up_key,
    up_value,
    window_out,
    latent_out,
):
    rows, part = tokens.shape
    tp_size, tp = lax.axis_size("tp"), lax.axis_index("tp")
    sp_size, sp = lax.axis_size("sp"), lax.axis_index("sp")
    top_bit = tp_size // 2
    half = rows // 2
    width = part * tp_size

    def near(block):
        blocks, bit = [block], 1
        while bit < top_bit:
            blocks = blocks + [swap(b, bit) for b in blocks]
            bit *= 2
        return blocks

    far_block = swap(tokens, top_bit)
    groups = [near(tokens), near(far_block)]
    projections = (down_latent, down_query, window_query, window_key, window_value, rotary_proj)
    joined = jnp.concatenate(projections, axis=1)

    squares, acc = None, None
    for g, blocks in enumerate(groups):
        starts = [(tp ^ (g * top_bit + k)) * part for k in range(top_bit)]
        weight = jnp.concatenate([lax.dynamic_slice_in_dim(joined, s, part, 0) for s in starts])
        gain = jnp.concatenate([lax.dynamic_slice_in_dim(norm_gain, s, part, 0) for s in starts])
        as_float = jnp.concatenate(blocks, axis=1).astype(F32)
        scaled = (as_float * gain[None, :]).astype(BF16)
        square = jnp.sum(as_float * as_float, axis=1)
        product = jnp.dot(scaled, weight, preferred_element_type=F32)
        squares = square if squares is None else squares + square
        acc = product if acc is None else acc + product
    row_scale = lax.rsqrt(squares / width + EPS)[:, None]
    outs, at = [], 0
    for weight in projections:
        outs.append((acc[:, at : at + weight.shape[1]] * row_scale).astype(BF16))
        at += weight.shape[1]
    latent_kv, latent_q, q_window, k_window, v_window, rotary_rows = outs

    first_pos = sp * rows
    positions = first_pos + jnp.arange(rows, dtype=jnp.int32)
    half_rope = ROPE // 2
    cosine, sine = angle_table(positions, half_rope)
    front, back = rotary_rows[:, :half_rope].astype(F32), rotary_rows[:, half_rope:].astype(F32)
    cos_k, sin_k = cosine.T, sine.T
    k_rot = jnp.concatenate(
        [
            front * cos_k - back * sin_k,
            back * cos_k + front * sin_k,
            jnp.zeros((rows, LANES - ROPE), F32),
        ],
        axis=1,
    ).astype(BF16)
    normed_kv = norm_rows(latent_kv, latent_gain)
    core = tp % 2
    kv_half = latent_kv.shape[1] // 2
    piece = lax.dynamic_slice_in_dim(normed_kv, core * kv_half, kv_half, 1)
    ring = [(i, (i + 2) % sp_size) for i in range(sp_size)]
    side = [(i, i ^ 1) for i in range(sp_size)]
    up_both = jnp.concatenate([up_key, up_value], axis=1)
    up_both = jnp.concatenate(
        [
            lax.dynamic_slice_in_dim(up_both, core * kv_half, kv_half, 0),
            lax.dynamic_slice_in_dim(up_both, (1 - core) * kv_half, kv_half, 0),
        ]
    )
    latent_heads = up_query.shape[1] // (NOPE + ROPE)
    pairs = latent_heads // 2
    payload = jnp.concatenate([piece, k_rot], axis=1)
    arrived = []
    for i in range(sp_size // 2):
        both = jnp.concatenate([payload, lax.ppermute(payload, "sp", side)], axis=0)
        arrived.append((both[:, :kv_half], swap(both[:, :kv_half], 1), both[:, kv_half:]))
        if i + 1 < sp_size // 2:
            payload = lax.ppermute(payload, "sp", ring)

    top_set = tp // top_bit
    other = 1 - top_set
    heads_dev = window_query.shape[1] // HD
    stacked = jnp.concatenate([k_window, v_window], axis=1)
    up = [(i, i + 1) for i in range(sp_size - 1)]
    down = [(i + 1, i) for i in range(sp_size - 1)]
    before = lax.ppermute(stacked[rows - WINDOW :], "sp", up)
    after = lax.ppermute(stacked[:WINDOW], "sp", down)
    padded = jnp.concatenate([before, stacked, after], axis=0)
    kv_width = k_window.shape[1]
    head_ids = tp * heads_dev + jnp.arange(heads_dev, dtype=jnp.int32)
    slopes = jnp.exp2(-8.0 * (head_ids.astype(F32) + 1.0) / A_HEADS)
    info = jnp.stack([other, top_set, first_pos, rows * sp_size]).astype(jnp.int32)
    out_window = window_attention(
        q_window, padded[:, :kv_width], padded[:, kv_width:], info, slopes, sink_logit
    )

    def reorder(x):
        return jnp.concatenate(
            [
                lax.dynamic_slice_in_dim(x, other * half, half, 0),
                lax.dynamic_slice_in_dim(x, top_set * half, half, 0),
            ],
            axis=0,
        )

    normed_q = norm_rows(reorder(latent_q), query_gain)
    q_t = lax.dot_general(
        up_query, normed_q, (((0,), (1,)), ((), ())), preferred_element_type=F32
    ).astype(BF16)
    q_t = q_t.reshape(latent_heads, NOPE + ROPE, rows)
    cos_q, sin_q = angle_table(reorder(positions), half_rope)
    q_front = q_t[:, NOPE : NOPE + half_rope].astype(F32)
    q_back = q_t[:, NOPE + half_rope :].astype(F32)
    q_rot = jnp.concatenate(
        [q_front * cos_q - q_back * sin_q, q_back * cos_q + q_front * sin_q], axis=1
    ).astype(BF16)
    zeros_head = jnp.zeros((NOPE, half), BF16)
    zeros_tail = jnp.zeros((LANES - ROPE, half), BF16)

    def columns(p, part_at):
        span = slice(part_at * half, (part_at + 1) * half)
        both = []
        for j in range(2):
            h = 2 * p + j
            nope = [q_t[h, :NOPE, span], zeros_head]
            both.append(
                jnp.concatenate(
                    (nope if j == 0 else nope[::-1]) + [q_rot[h, :, span], zeros_tail], axis=0
                )
            )
        return jnp.concatenate(both, axis=1)

    q_cols = jnp.concatenate(
        [columns(p, at) for at in range(2) for p in range(pairs)], axis=1
    )
    lat_scale = (NOPE + ROPE) ** (-0.5)
    lane = lax.broadcasted_iota(jnp.int32, (half, LANES), 1)
    halves = [[], []]
    state = None
    for i, (mine, theirs, rot) in enumerate(arrived):
        expanded = jnp.dot(
            jnp.concatenate([mine, theirs], axis=1), up_both, preferred_element_type=F32
        ).astype(BF16)
        keys, values = expanded[:, : pairs * LANES], expanded[:, pairs * LANES :]
        args = (keys, rot, values, q_cols, state, pairs, rows, lat_scale)
        if i + 1 < len(arrived):
            state = flash(*args)
            continue
        size = q_cols.shape[1] // 2
        for at in range(2):
            r = flash(*args, base=at * size, cols=size)
            for p in range(pairs):
                start = p * 2 * half
                first, second = r[start : start + half], r[start + half : start + 2 * half]
                halves[at].append(jnp.where(lane < VD, first, second))

    weight_out = jnp.concatenate([window_out, latent_out], axis=0)

    def project(x):
        return jnp.dot(x, weight_out, preferred_element_type=F32).astype(BF16)

    def reduce_near(x):
        bit = top_bit // 2
        if bit == 0:
            return project(x).astype(F32)
        count = x.shape[0] // 2
        mine = (tp // bit) % 2
        sent = project(lax.dynamic_slice_in_dim(x, (1 - mine) * count, count, 0))
        got = swap(sent, bit)
        total = project(lax.dynamic_slice_in_dim(x, mine * count, count, 0)).astype(F32)
        total = total + got.astype(F32)
        bit //= 2
        while bit:
            count //= 2
            mine = (tp // bit) % 2
            sent = lax.dynamic_slice_in_dim(total, (1 - mine) * count, count, 0).astype(BF16)
            total = lax.dynamic_slice_in_dim(total, mine * count, count, 0)
            total = total + swap(sent, bit).astype(F32)
            bit //= 2
        return total

    inputs = [
        jnp.concatenate([out_window[at * half : (at + 1) * half]] + halves[at], axis=1)
        for at in range(2)
    ]
    far_total = swap(reduce_near(inputs[0]).astype(BF16), top_bit)
    return (reduce_near(inputs[1]) + far_total.astype(F32)).astype(BF16)


def solution(mesh):
    placed = (
        P("sp", "tp"),
        P(),
        P(None, "tp"),
        P(None, "tp"),
        P(None, "tp"),
        P("tp"),
        P(),
        P(),
        P(),
        P(),
        P(),
        P(None, "tp"),
        P(None, "tp"),
        P(None, "tp"),
        P("tp", None),
        P("tp", None),
    )
    return jax.shard_map(
        per_device, mesh=mesh, in_specs=placed, out_specs=P(("sp", "tp"), None), check_vma=False
    )
```
